32 devices in a mesh: tp: 8 (over z, y), dp: 4 (over x, core).
Axes of the slice: x: 2, y: 2, z: 4, core: 2. Of those that a mesh axis runs over, the one named last changes fastest.
Arguments:
- incoming_token: bfloat16 [128, 4096], P(None, 'dp'), may hold values from -60 to 60
- input_norm_gain: float32 [2, 4096], P(None, 'dp'), may hold values from 0.1 to 1.9
- receptance_weight: bfloat16 [2, 4096, 8192], P(None, 'dp', 'tp'), may hold values from -0.09375 to 0.09375
- key_weight: bfloat16 [2, 4096, 8192], P(None, 'dp', 'tp'), may hold values from -0.09375 to 0.09375
- value_weight: bfloat16 [2, 4096, 8192], P(None, 'dp', 'tp'), may hold values from -0.09375 to 0.09375
- decay_weight: bfloat16 [2, 4096, 8192], P(None, 'dp', 'tp'), may hold values from -0.09375 to 0.09375
- learning_rate_weight: bfloat16 [2, 4096, 8192], P(None, 'dp', 'tp'), may hold values from -0.09375 to 0.09375
- gate_weight: bfloat16 [2, 4096, 8192], P(None, 'dp', 'tp'), may hold values from -0.09375 to 0.09375
- channel_decay_floor: float32 [2, 8192], P(None, 'tp'), may hold values from -5 to 2
- direct_token_weight: float32 [2, 8192], P(None, 'tp'), may hold values from -0.6 to 0.6
- head_norm_gain: float32 [2, 8192], P(None, 'tp'), may hold values from 0.1 to 1.9
- output_weight: bfloat16 [2, 8192, 4096], P(None, 'tp', 'dp'), may hold values from -0.0625 to 0.0625
- incoming_state: float32 [2, 128, 128, 64, 64], P(None, 'dp', 'tp'), may hold values from -6 to 6
Outputs:
- hidden_out: bfloat16 [128, 4096], P(None, 'dp')
- state_out: float32 [2, 128, 128, 64, 64], P(None, 'dp', 'tp')
The draws below stay inside these ranges and needn't reach their ends.
All inputs are finite; a program needn't handle non-finite values.
Results may differ from the reference program's by a relative error of at most 0.0053.
Values may be sent and summed in bfloat16 or wider, within the bound.
A program may use at most 192 MiB of HBM per device.

```python
import jax
import jax.numpy as jnp
from jax import lax

D = 4096
HEADS = 128
HEAD_CHANNELS = 64
MIXER_WIDTH = 8192
BATCH = 128


def draw_incoming_token(key, part):
    key_base = jax.random.fold_in(key, 11)
    key_rows = jax.random.fold_in(key, 12)
    column_rise = jnp.exp(jnp.log(3.0) * jnp.arange(D, dtype=jnp.float32) / (D - 1))
    base_draw = jnp.clip(jax.random.normal(key_base, (BATCH, D), jnp.float32), -4.0, 4.0)
    row_scale = jnp.exp(jax.random.uniform(key_rows, (BATCH, 1), jnp.float32, 0.0, jnp.log(10.0)))
    return (0.5 * base_draw * row_scale * column_rise[None, :]).astype(jnp.bfloat16)


def level_of(key, shape, shards, least, top_value):
    level = 1.0
    for axis_at, blocks in shards:
        steps = jax.random.uniform(jax.random.fold_in(jax.random.fold_in(key, 6), axis_at), (blocks,), jnp.float32, least / len(shards), top_value / len(shards))
        level = level * jnp.repeat(jnp.exp(steps), shape[axis_at] // blocks).reshape((-1,) + (1,) * (len(shape) - 1 - axis_at))
    return level


def gaussian(key, dims, deviation, limit, pieces=(), kind=jnp.bfloat16):
    result = jax.random.normal(key, dims, jnp.float32) * deviation
    if len(pieces) > 0:
        result = level_of(key, dims, pieces, -0.22, 0.18) * result
    return jnp.clip(result, min=-limit, max=limit).astype(kind)


def setup_inputs(seed: int = 0) -> dict:
    arg_keys = jax.random.split(jax.random.key(seed), 14)
    return {
        "incoming_token": draw_incoming_token(jax.random.fold_in(arg_keys[13], 71), 0),
        "input_norm_gain": jnp.clip(1.0 + 0.18 * jax.random.normal(arg_keys[1], (2, D), jnp.float32), 0.1, 1.9),
        "receptance_weight": gaussian(arg_keys[2], (2, D, MIXER_WIDTH), D ** -0.5, 0.09375, ((1, 4), (2, 8))),
        "key_weight": gaussian(arg_keys[3], (2, D, MIXER_WIDTH), D ** -0.5, 0.09375, ((1, 4), (2, 8))),
        "value_weight": gaussian(arg_keys[4], (2, D, MIXER_WIDTH), D ** -0.5, 0.09375, ((1, 4), (2, 8))),
        "decay_weight": gaussian(arg_keys[5], (2, D, MIXER_WIDTH), D ** -0.5, 0.09375, ((1, 4), (2, 8))),
        "learning_rate_weight": gaussian(arg_keys[6], (2, D, MIXER_WIDTH), D ** -0.5, 0.09375, ((1, 4), (2, 8))),
        "gate_weight": gaussian(arg_keys[7], (2, D, MIXER_WIDTH), D ** -0.5, 0.09375, ((1, 4), (2, 8))),
        "channel_decay_floor": jnp.clip(-5.0 + 7.0 * jax.random.uniform(arg_keys[8], (2, MIXER_WIDTH), jnp.float32) ** level_of(arg_keys[8], (2, MIXER_WIDTH), ((1, 8),), -0.2, 0.2), -5.0, 2.0),
        "direct_token_weight": gaussian(arg_keys[9], (2, MIXER_WIDTH), 0.1, 0.6, ((1, 8),), jnp.float32),
        "head_norm_gain": jnp.clip(1.0 + 0.18 * jax.random.normal(arg_keys[10], (2, MIXER_WIDTH), jnp.float32), 0.1, 1.9),
        "output_weight": gaussian(arg_keys[11], (2, MIXER_WIDTH, D), MIXER_WIDTH ** -0.5, 0.0625, ((1, 8), (2, 4))),
        "incoming_state": gaussian(arg_keys[12], (2, BATCH, HEADS, HEAD_CHANNELS, HEAD_CHANNELS), 1.0, 6.0, ((1, 4), (2, 8)), jnp.float32),
    }


def recurrent_mix_heads(projected_output, earlier_state, channel_decay_floor, direct_token_weight, head_norm_gain):
    step_count = projected_output.shape[0]
    local_heads = channel_decay_floor.shape[0] // HEAD_CHANNELS
    sections = projected_output.reshape(step_count, 6, local_heads, HEAD_CHANNELS)
    receptance_rows, keyvec, value_vector, pre_decay, pre_rate, pre_gate = [sections[:, part_index] for part_index in range(6)]
    decay_pre = channel_decay_floor.reshape(local_heads, HEAD_CHANNELS) + pre_decay
    decay_factor = jnp.exp(-jnp.exp(-jax.nn.softplus(-decay_pre) - 0.5))
    learn_rate = jax.nn.sigmoid(pre_rate)
    output_gate_value = jax.nn.sigmoid(pre_gate)
    unit_key = keyvec * lax.rsqrt(lax.optimization_barrier(jnp.sum(keyvec * keyvec, axis=-1, keepdims=True)) + 1e-06)
    rescaled_key = keyvec * learn_rate
    removed = -jnp.einsum('shvk,shk->shv', earlier_state, unit_key, precision=lax.Precision.HIGHEST)
    refreshed_state = earlier_state * decay_factor[:, :, None, :] + removed[..., None] * (unit_key * learn_rate)[:, :, None, :] + value_vector[..., None] * rescaled_key[:, :, None, :]
    readout = jnp.einsum('shvk,shk->shv', refreshed_state, receptance_rows, precision=lax.Precision.HIGHEST)
    group_mean = lax.optimization_barrier(jnp.mean(readout, axis=-1, keepdims=True))
    group_var = lax.optimization_barrier(jnp.mean(jnp.square(readout - group_mean), axis=-1, keepdims=True))
    normalized_input = (readout - group_mean) * lax.rsqrt(group_var + 0.00064) * head_norm_gain.reshape(local_heads, HEAD_CHANNELS)
    direct_token_term = lax.optimization_barrier(jnp.sum(receptance_rows * rescaled_key * direct_token_weight.reshape(local_heads, HEAD_CHANNELS), axis=-1, keepdims=True)) * value_vector
    mixer_output = ((normalized_input + direct_token_term) * output_gate_value).reshape(step_count, local_heads * HEAD_CHANNELS).astype(jnp.bfloat16)
    return (mixer_output, refreshed_state)

def reference(incoming_token, input_norm_gain, receptance_weight, key_weight, value_weight, decay_weight, learning_rate_weight, gate_weight, channel_decay_floor, direct_token_weight, head_norm_gain, output_weight, incoming_state):
    hidden = incoming_token
    new_states = []
    for block_index in range(2):
        hidden_wide = hidden.astype(jnp.float32)
        mean_square = lax.optimization_barrier(jnp.mean(hidden_wide * hidden_wide, axis=-1, keepdims=True))
        scaled_in = (hidden_wide * input_norm_gain[block_index]).astype(jnp.bfloat16)
        matrices = (receptance_weight, key_weight, value_weight, decay_weight, learning_rate_weight, gate_weight)
        projected_output = jnp.concatenate([jnp.dot(scaled_in, matrix[block_index], preferred_element_type=jnp.float32) for matrix in matrices], axis=-1) * lax.rsqrt(mean_square + 1e-06)

        def per_sequence(state_output_pair):
            mixer_output, refreshed_state = recurrent_mix_heads(state_output_pair[0][None], state_output_pair[1][None], channel_decay_floor[block_index], direct_token_weight[block_index], head_norm_gain[block_index])
            return (mixer_output[0], refreshed_state[0])
        mixer_output, refreshed_state = lax.map(per_sequence, (projected_output, incoming_state[block_index]))
        new_states.append(refreshed_state)
        branch = jnp.dot(mixer_output, output_weight[block_index], preferred_element_type=jnp.float32)
        hidden = (hidden_wide + branch).astype(jnp.bfloat16)
    return (hidden, jnp.stack(new_states))
```

```python
import functools

import jax
import jax.numpy as jnp
from jax import lax
from jax.experimental import pallas as pl
from jax.experimental.pallas import tpu as pltpu
from jax.sharding import PartitionSpec as P

HEAD_CHANNELS = 64
NT = (((1,), (1,)), ((), ()))
TN = (((0,), (0,)), ((), ()))
VMEM = pl.BlockSpec(memory_space=pltpu.VMEM)
ANY = pl.BlockSpec(memory_space=pl.ANY)


def remote(src, dst, send, recv, axis, to):
    return pltpu.make_async_remote_copy(
        src_ref=src,
        dst_ref=dst,
        send_sem=send,
        recv_sem=recv,
        device_id={axis: to},
        device_id_type=pl.DeviceIdType.MESH,
    )


def greet(sizes):
    barrier = pltpu.get_barrier_semaphore()
    count = 0
    for axis, size in sizes:
        me = lax.axis_index(axis)
        for step in range(1, size):
            pl.semaphore_signal(
                barrier,
                inc=1,
                device_id={axis: lax.rem(me + step, size)},
                device_id_type=pl.DeviceIdType.MESH,
            )
            count += 1
    pl.semaphore_wait(barrier, count)


def project_kernel(
    block, n, hidden, gain, w0, w1, w2, w3, w4, w5, out,
    wbuf, keep, send1, recv1, send2, recv2, squares, squares_in,
    wsem, s1, r1, s2, r2, sq_s, sq_r,
):
    weights = (w0, w1, w2, w3, w4, w5)
    batch, depth = hidden.shape
    rows = batch // n
    chips = n // 2
    loads = [
        pltpu.make_async_copy(w.at[block], wbuf.at[p], wsem.at[p]) for p, w in enumerate(weights)
    ]
    for load in loads:
        load.start()
    me = lax.axis_index("dp")
    core = lax.rem(me, 2)
    chip = lax.div(me, 2)
    partner = me + 1 - 2 * core
    wide = hidden[...].astype(jnp.float32)
    total = jnp.sum(wide * wide, axis=1, keepdims=True)
    squares[...] = jnp.broadcast_to(total, (batch, 128)).reshape(n, rows, 128)
    scaled = (wide * gain[block : block + 1, :]).astype(jnp.bfloat16)
    greet((("dp", n),))
    square_copies = []
    for j in range(1, n):
        to = lax.rem(me + j, n)
        copy = remote(squares.at[to], squares_in.at[j], sq_s.at[j], sq_r.at[j], "dp", to)
        copy.start()
        square_copies.append(copy)
    first = []
    second = []

    def cross(p):
        first[p].wait_recv()
        both = keep[p] + recv1[p].astype(jnp.float32)
        keep[p] = both
        send2[p] = both.astype(jnp.bfloat16)
        for j in range(1, chips):
            to = lax.rem(chip + j, chips)
            copy = remote(
                send2.at[p, to], recv2.at[p, j], s2.at[p, j], r2.at[p, j], "dp", 2 * to + core
            )
            copy.start()
            second.append((p, j, copy))

    for p in range(6):
        loads[p].wait()
        part = jnp.dot(scaled, wbuf[p], preferred_element_type=jnp.float32)
        part = part.reshape(chips, 2, rows, part.shape[1])
        even, odd = part[:, 0], part[:, 1]
        keep[p] = jnp.where(core == 0, even, odd)
        send1[p] = jnp.where(core == 0, odd, even).astype(jnp.bfloat16)
        copy = remote(send1.at[p], recv1.at[p], s1.at[p], r1.at[p], "dp", partner)
        copy.start()
        first.append(copy)
        if p >= 1:
            cross(p - 1)
    cross(5)
    mine = squares[me]
    for j, copy in enumerate(square_copies):
        copy.wait_recv()
        mine = mine + squares_in[j + 1]
    scale = lax.rsqrt(mine[:, :1] / (depth * n) + 1e-06)
    for p in range(6):
        value = keep[p, chip]
        for q, j, copy in second:
            if q == p:
                copy.wait_recv()
                value = value + recv2[p, j].astype(jnp.float32)
        out[p] = value * scale
    for copy in square_copies + first + [c for _, _, c in second]:
        copy.wait_send()


def project(block, n, hidden, gain, weights):
    batch, depth = hidden.shape
    width = weights[0].shape[2]
    rows, chips = batch // n, n // 2
    dma = pltpu.SemaphoreType.DMA
    return pl.pallas_call(
        functools.partial(project_kernel, block, n),
        out_shape=jax.ShapeDtypeStruct((6, rows, width), jnp.float32),
        in_specs=[VMEM, VMEM] + [ANY] * 6,
        out_specs=VMEM,
        scratch_shapes=[
            pltpu.VMEM((6, depth, width), jnp.bfloat16),
            pltpu.VMEM((6, chips, rows, width), jnp.float32),
            pltpu.VMEM((6, chips, rows, width), jnp.bfloat16),
            pltpu.VMEM((6, chips, rows, width), jnp.bfloat16),
            pltpu.VMEM((6, chips, rows, width), jnp.bfloat16),
            pltpu.VMEM((6, chips, rows, width), jnp.bfloat16),
            pltpu.VMEM((n, rows, 128), jnp.float32),
            pltpu.VMEM((n, rows, 128), jnp.float32),
            dma((6,)), dma((6,)), dma((6,)), dma((6, chips)), dma((6, chips)), dma((n,)), dma((n,)),
        ],
        compiler_params=pltpu.CompilerParams(collective_id=2 * block, has_side_effects=True),
        name=f"project{block}",
    )(hidden, gain, *weights)


def head_sums(value, ones):
    step = ones.shape[0]
    return jnp.concatenate(
        [
            jnp.dot(
                value[:, at : at + step],
                ones,
                preferred_element_type=jnp.float32,
                precision=lax.Precision.HIGHEST,
            )
            for at in range(0, value.shape[1], step)
        ],
        axis=1,
    )


def mix_kernel(block, steps, aliased, *refs):
    proj, floor, direct, norm_gain, state = refs[:5]
    out, mixed, ab, kr_heads, decay_heads, v_rows, krr_rows, y_rows = refs[5 + aliased :]
    at = pl.program_id(0)
    group, heads = state.shape[1:3]
    width = heads * HEAD_CHANNELS
    span = min(128, width)
    ones = (
        lax.broadcasted_iota(jnp.int32, (span, span), 0) // HEAD_CHANNELS
        == lax.broadcasted_iota(jnp.int32, (span, span), 1) // HEAD_CHANNELS
    ).astype(jnp.float32)

    @pl.when(at == 0)
    def _():
        r, k, v, pd, pa = proj[0], proj[1], proj[2], proj[3], proj[4]
        decay = jnp.exp(-jnp.exp(-jax.nn.softplus(-(floor[block : block + 1, :] + pd)) - 0.5))
        kr = k * jax.nn.sigmoid(pa)
        a = k / (head_sums(k * k, ones) + 1e-06)
        b = decay * r
        v_rows[...] = v
        krr_rows[...] = head_sums(kr * r, ones)
        for h in range(heads):
            cut = slice(h * HEAD_CHANNELS, (h + 1) * HEAD_CHANNELS)
            ab[:, h, :] = a[:, cut]
            ab[:, heads + h, :] = b[:, cut]
            kr_heads[:, h, :] = kr[:, cut]
            decay_heads[:, h, :] = decay[:, cut]

    own = (
        lax.broadcasted_iota(jnp.int32, (heads, width), 0)
        == lax.broadcasted_iota(jnp.int32, (heads, width), 1) // HEAD_CHANNELS
    )
    for s in range(group):
        row = at * group + s
        flat = state[0, s].reshape(width, HEAD_CHANNELS)
        both = lax.dot_general(
            ab[row].astype(jnp.bfloat16),
            flat.astype(jnp.bfloat16),
            NT,
            preferred_element_type=jnp.float32,
        )
        removed = jnp.sum(jnp.where(own, both[:heads], 0.0), axis=0, keepdims=True)
        kept = jnp.sum(jnp.where(own, both[heads:], 0.0), axis=0, keepdims=True)
        added = v_rows[pl.ds(row, 1), :] - removed
        y_rows[pl.ds(row, 1), :] = kept + added * krr_rows[pl.ds(row, 1), :]
        spread = jnp.where(own, added, 0.0).astype(jnp.bfloat16)
        outer = lax.dot_general(
            spread, kr_heads[row].astype(jnp.bfloat16), TN, preferred_element_type=jnp.float32
        )
        old = flat.reshape(heads, HEAD_CHANNELS, HEAD_CHANNELS)
        out[0, s] = old * decay_heads[row][:, None, :] + outer.reshape(old.shape)

    @pl.when(at == steps - 1)
    def _():
        y = y_rows[...]
        centred = y - head_sums(y, ones) / HEAD_CHANNELS
        var = head_sums(centred * centred, ones) / HEAD_CHANNELS
        r, k, v, pa, pg = proj[0], proj[1], proj[2], proj[4], proj[5]
        kr = k * jax.nn.sigmoid(pa)
        term = head_sums(r * kr * direct[block : block + 1, :], ones) * v
        normed = centred * lax.rsqrt(var + 0.00064) * norm_gain[block : block + 1, :]
        mixed[...] = ((normed + term) * jax.nn.sigmoid(pg)).astype(jnp.bfloat16)


def mix(block, proj, floor, direct, norm_gain, state, earlier):
    blocks, rows, heads = state.shape[:3]
    width = heads * HEAD_CHANNELS
    group = 4
    steps = rows // group
    aliased = earlier is not None
    tile = pl.BlockSpec(
        (1, group, heads, HEAD_CHANNELS, HEAD_CHANNELS), lambda i: (block, i, 0, 0, 0)
    )
    whole = lambda shape: pl.BlockSpec(shape, lambda i: (0,) * len(shape))
    f32 = jnp.float32
    return pl.pallas_call(
        functools.partial(mix_kernel, block, steps, int(aliased)),
        grid=(steps,),
        out_shape=(
            jax.ShapeDtypeStruct(state.shape, f32),
            jax.ShapeDtypeStruct((rows, width), jnp.bfloat16),
        ),
        in_specs=[whole(proj.shape)] + [whole((blocks, width))] * 3 + [tile] + [ANY] * aliased,
        out_specs=(tile, whole((rows, width))),
        scratch_shapes=[
            pltpu.VMEM((rows, 2 * heads, HEAD_CHANNELS), f32),
            pltpu.VMEM((rows, heads, HEAD_CHANNELS), f32),
            pltpu.VMEM((rows, heads, HEAD_CHANNELS), f32),
            pltpu.VMEM((rows, width), f32),
            pltpu.VMEM((rows, width), f32),
            pltpu.VMEM((rows, width), f32),
        ],
        input_output_aliases={5: 0} if aliased else {},
        compiler_params=pltpu.CompilerParams(dimension_semantics=("arbitrary",)),
        name=f"mix{block}",
    )(proj, floor, direct, norm_gain, state, *([earlier] if aliased else []))


def merge_kernel(
    block, n, nt, mixed, hidden, weight, out,
    wbuf, gathered, partial, send, recv, fresh, landed, wsem, gs, gr, rs_s, rs_r, ag_s, ag_r,
):
    load = pltpu.make_async_copy(weight.at[block], wbuf, wsem)
    load.start()
    batch, cols = hidden.shape
    rows, slab = batch // n, batch // nt
    me, rank = lax.axis_index("dp"), lax.axis_index("tp")
    greet((("dp", n), ("tp", nt)))
    gathers = []
    for j in range(1, n):
        to = lax.rem(me + j, n)
        gathers.append(remote(mixed, gathered.at[me], gs.at[j], gr.at[j], "dp", to))
    for copy in gathers:
        copy.start()
    gathered[me] = mixed[...]
    load.wait()
    for copy in gathers:
        copy.wait_recv()
    product = jnp.dot(
        gathered[...].reshape(batch, mixed.shape[1]), wbuf[...], preferred_element_type=jnp.float32
    ).reshape(nt, slab, cols)
    partial[...] = product
    send[...] = product.astype(jnp.bfloat16)
    scatters = []
    for j in range(1, nt):
        to = lax.rem(rank + j, nt)
        scatters.append(remote(send.at[to], recv.at[j], rs_s.at[j], rs_r.at[j], "tp", to))
    for copy in scatters:
        copy.start()
    start = pl.multiple_of(rank * slab, slab)
    value = hidden[pl.ds(start, slab), :].astype(jnp.float32) + partial[rank]
    for j, copy in enumerate(scatters):
        copy.wait_recv()
        value = value + recv[j + 1].astype(jnp.float32)
    fresh[...] = value.astype(jnp.bfloat16)
    spreads = []
    for j in range(1, nt):
        to = lax.rem(rank + j, nt)
        spreads.append(remote(fresh, landed.at[rank], ag_s.at[j], ag_r.at[j], "tp", to))
    for copy in spreads:
        copy.start()
    landed[rank] = value.astype(jnp.bfloat16)
    for copy in spreads:
        copy.wait_recv()
    out[...] = landed[...].reshape(batch, cols)
    for copy in gathers + scatters + spreads:
        copy.wait_send()


def merge(block, n, nt, mixed, hidden, weight):
    batch, cols = hidden.shape
    rows, width = mixed.shape
    slab = batch // nt
    if slab % 16:
        branch = jnp.dot(
            lax.all_gather(mixed, "dp", axis=0, tiled=True),
            weight[block],
            preferred_element_type=jnp.float32,
        )
        return (hidden.astype(jnp.float32) + lax.psum(branch, "tp")).astype(jnp.bfloat16)
    dma = pltpu.SemaphoreType.DMA
    bf16 = jnp.bfloat16
    return pl.pallas_call(
        functools.partial(merge_kernel, block, n, nt),
        out_shape=jax.ShapeDtypeStruct((batch, cols), bf16),
        in_specs=[VMEM, VMEM, ANY],
        out_specs=VMEM,
        scratch_shapes=[
            pltpu.VMEM((width, cols), bf16),
            pltpu.VMEM((n, rows, width), bf16),
            pltpu.VMEM((nt, slab, cols), jnp.float32),
            pltpu.VMEM((nt, slab, cols), bf16),
            pltpu.VMEM((nt, slab, cols), bf16),
            pltpu.VMEM((slab, cols), bf16),
            pltpu.VMEM((nt, slab, cols), bf16),
            dma, dma((n,)), dma((n,)), dma((nt,)), dma((nt,)), dma((nt,)), dma((nt,)),
        ],
        compiler_params=pltpu.CompilerParams(collective_id=2 * block + 1, has_side_effects=True),
        name=f"merge{block}",
    )(mixed, hidden, weight)


def solution(mesh):
    n, nt = mesh.shape["dp"], mesh.shape["tp"]

    def per_device(token, gain, wr, wk, wv, wd, wa, wg, floor, direct, norm_gain, wo, state):
        hidden, states = token, None
        for block in range(state.shape[0]):
            proj = project(block, n, hidden, gain, (wr, wk, wv, wd, wa, wg))
            states, mixed = mix(block, proj, floor, direct, norm_gain, state, states)
            hidden = merge(block, n, nt, mixed, hidden, wo)
        return hidden, states

    return jax.shard_map(
        per_device,
        mesh=mesh,
        in_specs=(
            P(None, "dp"),
            P(None, "dp"),
            *[P(None, "dp", "tp")] * 6,
            *[P(None, "tp")] * 3,
            P(None, "tp", "dp"),
            P(None, "dp", "tp", None, None),
        ),
        out_specs=(P(None, "dp"), P(None, "dp", "tp", None, None)),
        check_vma=False,
    )
```
